32 devices in a mesh: fs: 8 (over z, y), tp: 4 (over x, core).
Axes of the slice: x: 2, y: 2, z: 4, core: 2. Of those that a mesh axis runs over, the one named last changes fastest.
Arguments:
- inputs: bfloat16 [4096, 2112], P('fs', 'tp'), may hold values from -6 to 6
- w_conv_up: bfloat16 [2112, 2816], P('fs', 'tp'), may hold values from -0.125 to 0.125
- w_gate_up: bfloat16 [2112, 2816], P('fs', 'tp'), may hold values from -0.125 to 0.125
- w_down: bfloat16 [2816, 2112], P('tp', 'fs'), may hold values from -0.109375 to 0.109375
- taps: float32 [3, 2816], replicated, may hold values from -3 to 3
- conv_bias: float32 [2816], replicated, may hold values from -3 to 3
- cotangent: bfloat16 [4096, 2112], P('fs', 'tp'), may hold values from -6 to 6
Outputs:
- grad_inputs: bfloat16 [4096, 2112], P('fs', 'tp')
- grad_conv_up: float32 [2112, 2816], P('fs', 'tp')
- unit_norms: float32 [2816], P('tp')
- grad_taps: float32 [3, 2816], replicated
- grad_bias: float32 [2816], replicated
The draws below stay inside these ranges and needn't reach their ends.
All inputs are finite; a program needn't handle non-finite values.
Results may differ from the reference program's by a relative error of at most 0.018.
Values may be sent and summed in bfloat16 or wider, within the bound.
A program may use at most 64 MiB of HBM per device.

```python
import math
import jax
import jax.numpy as jnp
from jax import lax

D = 2112
FF = 2816
TAPS = 3
TOKENS = 4096
N_TP = 4


def with_spikes(entries, key, source, target, shards_of, factor):
    def block_of(dim):
        return (jnp.arange(entries.shape[dim]) // (entries.shape[dim] // shards_of)).reshape((-1,) + (1,) * (entries.ndim - 1 - dim))

    near = jax.random.permutation(key, shards_of)[block_of(target)]
    other_side = (block_of(target) + shards_of // 2) % shards_of
    return jnp.where((block_of(source) == near) | (block_of(source) == other_side), factor * entries, entries)


def shard_levels(key, extent, split, smallest, high):
    def one(dim, blocks):
        steps = jax.random.uniform(jax.random.fold_in(jax.random.fold_in(key, 6), dim), (blocks,), jnp.float32, smallest / len(split), high / len(split))
        return jnp.repeat(jnp.exp(steps), extent[dim] // blocks).reshape((-1,) + (1,) * (len(extent) - dim - 1))

    level = one(*split[0])
    for cut in split[1:]:
        level = level * one(*cut)
    return level


def gaussian(own_key, dims, scale, reach, cuts=(), kind=jnp.bfloat16):
    level = shard_levels(own_key, dims, cuts, -0.22, 0.18) if cuts else 1.0
    result = jax.random.normal(own_key, dims, jnp.float32) * scale * level
    return jnp.minimum(jnp.maximum(result, -reach), reach).astype(kind)


def heavy_noise(stream_key, extent, deviation, limit, cuts, heavy, held_as=jnp.bfloat16):
    entries = deviation * jax.random.normal(stream_key, extent, jnp.float32)
    if cuts:
        entries = entries * shard_levels(stream_key, extent, cuts, -0.22, 0.18)
    return jnp.clip(with_spikes(entries, jax.random.fold_in(stream_key, 3), *heavy), -limit, limit).astype(held_as)


def setup_inputs(seed: int = 0) -> dict:
    key_list = jax.random.split(jax.random.key(seed), 8)
    return {
        "inputs": heavy_noise(key_list[0], (TOKENS, D), 1.0, 6.0, ((0, 8), (1, 4)), (0, 1, 8, 2.0)),
        "w_conv_up": gaussian(key_list[1], (D, FF), D ** -0.5, 0.125, ((0, 8), (1, 4))),
        "w_gate_up": gaussian(key_list[2], (D, FF), D ** -0.5, 0.125, ((0, 8), (1, 4))),
        "w_down": gaussian(key_list[3], (FF, D), FF ** -0.5, 0.109375, ((0, 4), (1, 8))),
        "taps": gaussian(key_list[4], (TAPS, FF), 0.6, 3.0, (), jnp.float32),
        "conv_bias": gaussian(key_list[5], (FF,), 0.5, 3.0, (), jnp.float32),
        "cotangent": gaussian(key_list[6], (TOKENS, D), 1.0, 6.0, ((0, 8), (1, 4))),
    }


def gelu_parts(value):
    normal_cdf = 0.5 * (1.0 + jax.scipy.special.erf(value / math.sqrt(2.0)))
    density = jnp.exp(-0.5 * value * value) / math.sqrt(2.0 * math.pi)
    return (value * normal_cdf, normal_cdf + value * density)

def reference(inputs, w_conv_up, w_gate_up, w_down, taps, conv_bias, cotangent):
    span = TAPS - 1
    rows = inputs.shape[0]
    up_a = jnp.dot(inputs, w_conv_up, preferred_element_type=jnp.float32).astype(jnp.bfloat16)
    up_b = jnp.dot(inputs, w_gate_up, preferred_element_type=jnp.float32).astype(jnp.bfloat16)
    extended = jnp.concatenate([jnp.zeros((span, FF), jnp.float32), up_a.astype(jnp.float32)], 0)
    conv_out = conv_bias[None, :] + sum((taps[i][None, :] * extended[i:i + rows] for i in range(TAPS)))
    d_hidden = jnp.dot(cotangent, w_down.T, preferred_element_type=jnp.float32).astype(jnp.bfloat16)
    gelu_value, gelu_slope = gelu_parts(conv_out)
    d_conv = d_hidden.astype(jnp.float32) * up_b.astype(jnp.float32) * gelu_slope
    d_up_b = (d_hidden.astype(jnp.float32) * gelu_value).astype(jnp.bfloat16)
    d_extended = jnp.concatenate([d_conv, jnp.zeros((span, FF), jnp.float32)], 0)
    d_up_a = sum((taps[i][None, :] * d_extended[span - i:span - i + rows] for i in range(TAPS))).astype(jnp.bfloat16)
    grad_taps = jnp.stack([lax.optimization_barrier(jnp.sum(d_conv * extended[i:i + rows], axis=0)) for i in range(TAPS)], 0)
    grad_bias = lax.optimization_barrier(jnp.sum(d_conv, axis=0))
    group = FF // N_TP
    total = jnp.zeros((rows, D), jnp.float32)
    for k in range(N_TP):
        lo = k * group
        part = jnp.dot(d_up_a[:, lo:lo + group], w_conv_up[:, lo:lo + group].T, preferred_element_type=jnp.float32)
        part = part + jnp.dot(d_up_b[:, lo:lo + group], w_gate_up[:, lo:lo + group].T, preferred_element_type=jnp.float32)
        total = total + part.astype(jnp.bfloat16).astype(jnp.float32)
    grad_inputs = total.astype(jnp.bfloat16)
    grad_conv_up = jnp.dot(inputs.T, d_up_a, preferred_element_type=jnp.float32)
    unit_norms = lax.optimization_barrier(jnp.sum(grad_conv_up * grad_conv_up, axis=0))
    return (grad_inputs, grad_conv_up, unit_norms, grad_taps, grad_bias)
```

```python
import functools
import math

import jax
import jax.numpy as jnp
from jax import lax
from jax.experimental import pallas as pl
from jax.experimental.pallas import tpu as pltpu
from jax.sharding import PartitionSpec as P

TAPS = 3
LANES = 128
MESH = pl.DeviceIdType.MESH
VMEM = pl.BlockSpec(memory_space=pltpu.VMEM)
ANY = pl.BlockSpec(memory_space=pl.ANY)


def shifted(block, axis, distance):
    devices = range(lax.axis_size(axis))
    route = [(i - distance, i) for i in devices if i - distance in devices]
    return lax.ppermute(block, axis, route)


def gelu_parts(value):
    normal_cdf = 0.5 * (1.0 + jax.scipy.special.erf(value / math.sqrt(2.0)))
    density = jnp.exp(-0.5 * value * value) / math.sqrt(2.0 * math.pi)
    return (value * normal_cdf, normal_cdf + value * density)


def with_collectives(inputs, w_conv_up, w_gate_up, w_down, taps, conv_bias, cotangent):
    span = TAPS - 1
    rows = inputs.shape[0]
    width = w_conv_up.shape[1]
    col_start = lax.axis_index("tp") * width
    taps_own = lax.dynamic_slice_in_dim(taps, col_start, width, 1)
    bias_own = lax.dynamic_slice_in_dim(conv_bias, col_start, width, 0)
    features, cot_full = (
        lax.all_gather(inputs, "tp", axis=1, tiled=True),
        lax.all_gather(cotangent, "tp", axis=1, tiled=True),
    )
    conv_weight, gate_weight = (
        lax.all_gather(w_conv_up, "fs", axis=0, tiled=True),
        lax.all_gather(w_gate_up, "fs", axis=0, tiled=True),
    )
    columns = cot_full
    d_hidden = lax.dot_general(
        columns,
        lax.all_gather(w_down, "fs", axis=1, tiled=True),
        (((1,), (1,)), ((), ())),
        preferred_element_type=jnp.float32,
    ).astype(jnp.bfloat16)
    up_a = jnp.dot(features, conv_weight, preferred_element_type=jnp.float32).astype(jnp.bfloat16)
    up_b = jnp.dot(features, gate_weight, preferred_element_type=jnp.float32).astype(jnp.bfloat16)
    earlier = shifted(up_a[rows - span :], "fs", 1)
    extended = jnp.concatenate([earlier, up_a], 0).astype(jnp.float32)
    conv_out = bias_own[None, :] + sum(
        (taps_own[i][None, :] * extended[i : i + rows] for i in range(TAPS))
    )
    gelu_value, gelu_slope = gelu_parts(conv_out)
    hidden_grad = d_hidden.astype(jnp.float32)
    d_conv = hidden_grad * up_b.astype(jnp.float32) * gelu_slope
    d_up_b = (hidden_grad * gelu_value).astype(jnp.bfloat16)
    later = shifted(d_conv[:span], "fs", -1)
    d_extended = jnp.concatenate([d_conv, later], 0)
    d_up_a = sum(
        (taps_own[i][None, :] * d_extended[span - i : span - i + rows] for i in range(TAPS))
    ).astype(jnp.bfloat16)
    tap_terms = [jnp.sum(d_conv * extended[i : i + rows], axis=0) for i in range(TAPS)]
    column_part = jnp.stack(tap_terms + [jnp.sum(d_conv, axis=0)], 0)
    contract = (((1,), (1,)), ((), ()))
    partial_sum = lax.dot_general(d_up_a, conv_weight, contract, preferred_element_type=jnp.float32)
    partial_sum = partial_sum + lax.dot_general(
        d_up_b, gate_weight, contract, preferred_element_type=jnp.float32
    )
    grad_inputs = lax.psum_scatter(
        partial_sum.astype(jnp.bfloat16), "tp", scatter_dimension=1, tiled=True
    )
    columns = features
    grad_conv_up = lax.psum_scatter(
        lax.dot_general(
            columns, d_up_a, (((0,), (0,)), ((), ())), preferred_element_type=jnp.float32
        ),
        "fs",
        scatter_dimension=0,
        tiled=True,
    )
    squares = jnp.sum(grad_conv_up * grad_conv_up, axis=0)
    placed = jnp.zeros((TAPS + 1, width * lax.axis_size("tp")), jnp.float32)
    placed = lax.dynamic_update_slice_in_dim(placed, column_part, col_start, 1)
    full_columns = lax.psum(placed, ("fs", "tp"))
    unit_norms = lax.psum(squares, "fs")
    return (grad_inputs, grad_conv_up, unit_norms, full_columns[:TAPS], full_columns[TAPS])


def ring_member(place, n):
    depth = n // 2
    place = lax.rem(place + 2 * n, n)
    side = place // depth
    along = lax.rem(place, depth)
    return (side * (depth - 1) + (1 - 2 * side) * along) * 2 + side


def ring_place(index, n):
    side = lax.rem(index, 2)
    along = index // 2
    return side * (n - 1 - 2 * along) + along


def greet(peers):
    barrier = pltpu.get_barrier_semaphore()
    for peer in peers:
        pl.semaphore_signal(barrier, inc=1, device_id=peer, device_id_type=MESH)
    pl.semaphore_wait(barrier, len(peers))


def gather_kernel(n, t, *refs):
    weights, tokens = refs[:6], refs[6:8]
    w_out, t_out = refs[8:14], refs[14:16]
    send_sem, recv_sem, t_send, t_recv, own_sem = refs[16:]
    me, mine = lax.axis_index("fs"), lax.axis_index("tp")
    place = ring_place(me, n)
    ways = (
        {"fs": ring_member(place + 1, n)},
        {"fs": ring_member(place - 1, n)},
    )
    peers = [{"tp": lax.rem(mine + k, t)} for k in range(1, t)]
    greet(list(ways) + peers)
    ring = []
    for step in range(n - 1):
        copies = []
        for i in range(6):
            way = i % 2
            if step:
                ring[step - 1][i].wait_recv()
            owner = ring_member(place - step if way == 0 else place + step, n)
            copy = pltpu.make_async_remote_copy(
                src_ref=w_out[i].at[owner] if step else weights[i],
                dst_ref=w_out[i].at[owner],
                send_sem=send_sem.at[step, i],
                recv_sem=recv_sem.at[step, i],
                device_id=ways[way],
                device_id_type=MESH,
            )
            copy.start()
            copies.append(copy)
        ring.append(copies)
        if step == 0:
            across = []
            for i in range(2):
                for k in range(1, t):
                    copy = pltpu.make_async_remote_copy(
                        src_ref=tokens[i],
                        dst_ref=t_out[i].at[mine],
                        send_sem=t_send.at[i, k - 1],
                        recv_sem=t_recv.at[i, k - 1],
                        device_id=peers[k - 1],
                        device_id_type=MESH,
                    )
                    copy.start()
                    across.append(copy)
            own = [
                pltpu.make_async_copy(weights[i], w_out[i].at[me], own_sem.at[i])
                for i in range(6)
            ] + [
                pltpu.make_async_copy(tokens[i], t_out[i].at[mine], own_sem.at[6 + i])
                for i in range(2)
            ]
            for copy in own:
                copy.start()
    for copy in ring[-1]:
        copy.wait_recv()
    for copy in across:
        copy.wait_recv()
    for copies in ring:
        for copy in copies:
            copy.wait_send()
    for copy in across:
        copy.wait_send()
    for copy in own:
        copy.wait()


def gather_all(weights, tokens, n, t):
    shape = jax.ShapeDtypeStruct
    return pl.pallas_call(
        functools.partial(gather_kernel, n, t),
        out_shape=[shape((n,) + w.shape, w.dtype) for w in weights]
        + [shape((t,) + x.shape, x.dtype) for x in tokens],
        in_specs=[VMEM] * 8,
        out_specs=[ANY] * 8,
        scratch_shapes=[
            pltpu.SemaphoreType.DMA((n - 1, 6)),
            pltpu.SemaphoreType.DMA((n - 1, 6)),
            pltpu.SemaphoreType.DMA((2, t - 1)),
            pltpu.SemaphoreType.DMA((2, t - 1)),
            pltpu.SemaphoreType.DMA((8,)),
        ],
        compiler_params=pltpu.CompilerParams(collective_id=0, has_side_effects=True),
        name="gather_all",
    )(*weights, *tokens)


def reduce_kernel(n, t, *refs):
    grads, partial, columns = refs[:2], refs[2], refs[3]
    g_out, i_out, norm_out, col_out = refs[4:6], refs[6], refs[7], refs[8]
    (sent, held, arrived, col_all, col_sum, norm_own, norm_all) = refs[9:16]
    (send_sem, recv_sem, t_send, t_recv, c_send, c_recv, s_send, s_recv, n_send, n_recv) = refs[16:]
    parts = grads[0].shape[1]
    me, mine = lax.axis_index("fs"), lax.axis_index("tp")
    place = ring_place(me, n)
    ways = (
        {"fs": ring_member(place + 1, n)},
        {"fs": ring_member(place - 1, n)},
    )
    peers = [{"tp": lax.rem(mine + k, t)} for k in range(1, t)]
    column = [{"fs": lax.rem(me + k, n)} for k in range(1, n)]
    greet(column + peers)

    def push(src, dst, send, recv, to):
        copy = pltpu.make_async_remote_copy(
            src_ref=src, dst_ref=dst, send_sem=send, recv_sem=recv,
            device_id=to, device_id_type=MESH,
        )
        copy.start()
        return copy

    col_pushes = [
        push(columns, col_all.at[me], c_send.at[k], c_recv.at[k], column[k])
        for k in range(n - 1)
    ]
    across = [
        push(
            partial.at[lax.rem(mine + k, t)],
            arrived.at[k - 1],
            t_send.at[k - 1],
            t_recv.at[k - 1],
            peers[k - 1],
        )
        for k in range(1, t)
    ]
    ring = []
    for step in range(n - 1):
        copies = []
        for c in range(parts):
            for way in range(2):
                ahead = place - 1 - step if way == 0 else place + 1 + step
                value = grads[way][ring_member(ahead, n), c]
                slot = c * 2 + way
                if step:
                    ring[step - 1][slot].wait_recv()
                    value = value + held[step - 1, slot].astype(jnp.float32)
                sent[step, slot] = value.astype(jnp.bfloat16)
                copies.append(
                    push(
                        sent.at[step, slot],
                        held.at[step, slot],
                        send_sem.at[step, slot],
                        recv_sem.at[step, slot],
                        ways[way],
                    )
                )
        ring.append(copies)
        if step == 1:
            for copy in col_pushes:
                copy.wait_recv()
            total = jnp.zeros(columns.shape, jnp.float32)
            for k in range(n):
                total = total + jnp.where(me == k, columns[...], col_all[k])
            col_sum[...] = total
            col_out[mine] = total
            sum_pushes = [
                push(col_sum, col_out.at[mine], s_send.at[k], s_recv.at[k], peers[k])
                for k in range(t - 1)
            ]
    half = norm_own.shape[1] // 2
    for way in range(2):
        squares = jnp.zeros((1, half), jnp.float32)
        for c in range(parts):
            slot = c * 2 + way
            ring[-1][slot].wait_recv()
            value = grads[way][me, c] + held[n - 2, slot].astype(jnp.float32)
            g_out[way][c] = value
            squares = squares + jnp.sum(value * value, axis=0, keepdims=True)
        norm_own[:, way * half : (way + 1) * half] = squares
    norm_pushes = [
        push(norm_own, norm_all.at[me], n_send.at[k], n_recv.at[k], column[k])
        for k in range(n - 1)
    ]
    for copy in across:
        copy.wait_recv()
    rows = partial.shape[1]
    piece = 16 if rows % 16 == 0 else 8

    @pl.loop(0, rows // piece)
    def _(r):
        at = pl.ds(pl.multiple_of(r * piece, piece), piece)
        total = partial[mine, at, :].astype(jnp.float32)
        for k in range(t - 1):
            total = total + arrived[k, at, :].astype(jnp.float32)
        i_out[at, :] = total.astype(jnp.bfloat16)

    for copy in norm_pushes:
        copy.wait_recv()
    total = jnp.zeros(norm_own.shape, jnp.float32)
    for k in range(n):
        total = total + jnp.where(me == k, norm_own[...], norm_all[k])
    norm_out[...] = total
    for copy in sum_pushes:
        copy.wait_recv()
    for copies in ring + [across, col_pushes, sum_pushes, norm_pushes]:
        for copy in copies:
            copy.wait_send()


def reduce_all(grads, partial, columns, n, t):
    shape = jax.ShapeDtypeStruct
    parts, rows, half = grads[0].shape[1:]
    dma = pltpu.SemaphoreType.DMA
    blocks = pltpu.VMEM((n - 1, 2 * parts, rows, half), jnp.bfloat16)
    return pl.pallas_call(
        functools.partial(reduce_kernel, n, t),
        out_shape=[shape((parts, rows, half), jnp.float32)] * 2
        + [
            shape(partial.shape[1:], jnp.bfloat16),
            shape((1, 2 * half), jnp.float32),
            shape((t,) + columns.shape, jnp.float32),
        ],
        in_specs=[VMEM] * 4,
        out_specs=[VMEM] * 5,
        scratch_shapes=[
            blocks,
            blocks,
            pltpu.VMEM((t - 1,) + partial.shape[1:], jnp.bfloat16),
            pltpu.VMEM((n,) + columns.shape, jnp.float32),
            pltpu.VMEM(columns.shape, jnp.float32),
            pltpu.VMEM((1, 2 * half), jnp.float32),
            pltpu.VMEM((n, 1, 2 * half), jnp.float32),
            dma((n - 1, 2 * parts)),
            dma((n - 1, 2 * parts)),
            dma((t - 1,)),
            dma((t - 1,)),
            dma((n - 1,)),
            dma((n - 1,)),
            dma((t - 1,)),
            dma((t - 1,)),
            dma((n - 1,)),
            dma((n - 1,)),
        ],
        compiler_params=pltpu.CompilerParams(
            collective_id=1, has_side_effects=True, vmem_limit_bytes=56 * 1024 * 1024
        ),
        name="reduce_all",
    )(*grads, partial, columns)


def split(array, half):
    array = jnp.pad(array, ((0, 0), (0, 2 * half - array.shape[1])))
    return [array[:, :half], array[:, half:]]


def with_kernels(inputs, w_conv_up, w_gate_up, w_down, taps, conv_bias, cotangent):
    n, t = lax.axis_size("fs"), lax.axis_size("tp")
    span = TAPS - 1
    rows = inputs.shape[0]
    shard, width = w_conv_up.shape
    half = -(-width // (2 * LANES)) * LANES
    col_start = lax.axis_index("tp") * width
    taps_own = jnp.pad(
        lax.dynamic_slice_in_dim(taps, col_start, width, 1), ((0, 0), (0, 2 * half - width))
    )
    bias_own = jnp.pad(
        lax.dynamic_slice_in_dim(conv_bias, col_start, width, 0), ((0, 2 * half - width),)
    )
    weights = [p for w in (w_down.T, w_conv_up, w_gate_up) for p in split(w, half)]
    got = gather_all(weights, [inputs.T, cotangent.T], n, t)
    down, conv, gate = [[g.reshape(n * shard, half) for g in got[i : i + 2]] for i in (0, 2, 4)]
    features, cot_full = [g.reshape(-1, rows) for g in got[6:]]

    def project(left, right):
        dots = [
            lax.dot_general(
                left, r, (((0,), (0,)), ((), ())), preferred_element_type=jnp.float32
            ).astype(jnp.bfloat16)
            for r in right
        ]
        return jnp.concatenate(dots, 1)

    up_a = project(features, conv)
    earlier = shifted(up_a[rows - span :], "fs", 1)
    d_hidden = project(cot_full, down)
    up_b = project(features, gate)
    extended = jnp.concatenate([earlier, up_a], 0).astype(jnp.float32)
    conv_out = bias_own[None, :] + sum(
        (taps_own[i][None, :] * extended[i : i + rows] for i in range(TAPS))
    )
    gelu_value, gelu_slope = gelu_parts(conv_out)
    hidden_grad = d_hidden.astype(jnp.float32)
    d_conv = hidden_grad * up_b.astype(jnp.float32) * gelu_slope
    d_up_b = (hidden_grad * gelu_value).astype(jnp.bfloat16)
    later = shifted(d_conv[:span], "fs", -1)
    d_extended = jnp.concatenate([d_conv, later], 0)
    d_up_a = sum(
        (taps_own[i][None, :] * d_extended[span - i : span - i + rows] for i in range(TAPS))
    ).astype(jnp.bfloat16)
    tap_terms = [jnp.sum(d_conv * extended[i : i + rows], axis=0) for i in range(TAPS)]
    column_part = jnp.stack(tap_terms + [jnp.sum(d_conv, axis=0)], 0)
    partial_sum = 0.0
    for weight, grad in ((conv, d_up_a), (gate, d_up_b)):
        for h in range(2):
            partial_sum = partial_sum + lax.dot_general(
                weight[h],
                grad[:, h * half : (h + 1) * half],
                (((1,), (1,)), ((), ())),
                preferred_element_type=jnp.float32,
            )
    partial = partial_sum.astype(jnp.bfloat16).reshape(t, -1, rows)
    parts = next(p for p in (3, 4, 2, 1) if shard % (8 * p) == 0)
    grads = [
        jnp.dot(
            features, d_up_a[:, h * half : (h + 1) * half], preferred_element_type=jnp.float32
        ).reshape(n, parts, shard // parts, half)
        for h in range(2)
    ]
    low, high, grad_inputs, norms, columns = reduce_all(grads, partial, column_part, n, t)
    grad_conv_up = jnp.concatenate(
        [low.reshape(shard, half), high.reshape(shard, half)[:, : width - half]], 1
    )
    full = columns[:, :, :width].transpose(1, 0, 2).reshape(TAPS + 1, t * width)
    return (grad_inputs.T, grad_conv_up, norms[0, :width], full[:TAPS], full[TAPS])


def per_device(inputs, w_conv_up, *rest):
    n, t = lax.axis_size("fs"), lax.axis_size("tp")
    aligned = w_conv_up.shape[0] % 8 == 0 and inputs.shape[1] % 8 == 0
    small = n % 2 == 0 and 4 <= n <= 16 and 2 <= t <= 8
    chosen = with_kernels if aligned and small else with_collectives
    return chosen(inputs, w_conv_up, *rest)


def solution(mesh):
    return jax.shard_map(
        per_device,
        mesh=mesh,
        in_specs=(
            P("fs", "tp"),
            P("fs", "tp"),
            P("fs", "tp"),
            P("tp", "fs"),
            P(),
            P(),
            P("fs", "tp"),
        ),
        out_specs=(P("fs", "tp"), P("fs", "tp"), P("tp"), P(), P()),
        check_vma=False,
    )
```

```python
import functools
import math

import jax
import jax.numpy as jnp
from jax import lax
from jax.experimental import pallas as pl
from jax.experimental.pallas import tpu as pltpu
from jax.sharding import PartitionSpec as P

TAPS = 3
LANES = 128
MESH = pl.DeviceIdType.MESH
VMEM = pl.BlockSpec(memory_space=pltpu.VMEM)
ANY = pl.BlockSpec(memory_space=pl.ANY)


def shifted(block, axis, distance):
    devices = range(lax.axis_size(axis))
    route = [(i - distance, i) for i in devices if i - distance in devices]
    return lax.ppermute(block, axis, route)


def gelu_parts(value):
    normal_cdf = 0.5 * (1.0 + jax.scipy.special.erf(value / math.sqrt(2.0)))
    density = jnp.exp(-0.5 * value * value) / math.sqrt(2.0 * math.pi)
    return (value * normal_cdf, normal_cdf + value * density)


def with_collectives(inputs, w_conv_up, w_gate_up, w_down, taps, conv_bias, cotangent):
    span = TAPS - 1
    rows = inputs.shape[0]
    width = w_conv_up.shape[1]
    col_start = lax.axis_index("tp") * width
    taps_own = lax.dynamic_slice_in_dim(taps, col_start, width, 1)
    bias_own = lax.dynamic_slice_in_dim(conv_bias, col_start, width, 0)
    features, cot_full = (
        lax.all_gather(inputs, "tp", axis=1, tiled=True),
        lax.all_gather(cotangent, "tp", axis=1, tiled=True),
    )
    conv_weight, gate_weight = (
        lax.all_gather(w_conv_up, "fs", axis=0, tiled=True),
        lax.all_gather(w_gate_up, "fs", axis=0, tiled=True),
    )
    columns = cot_full
    d_hidden = lax.dot_general(
        columns,
        lax.all_gather(w_down, "fs", axis=1, tiled=True),
        (((1,), (1,)), ((), ())),
        preferred_element_type=jnp.float32,
    ).astype(jnp.bfloat16)
    up_a = jnp.dot(features, conv_weight, preferred_element_type=jnp.float32).astype(jnp.bfloat16)
    up_b = jnp.dot(features, gate_weight, preferred_element_type=jnp.float32).astype(jnp.bfloat16)
    earlier = shifted(up_a[rows - span :], "fs", 1)
    extended = jnp.concatenate([earlier, up_a], 0).astype(jnp.float32)
    conv_out = bias_own[None, :] + sum(
        (taps_own[i][None, :] * extended[i : i + rows] for i in range(TAPS))
    )
    gelu_value, gelu_slope = gelu_parts(conv_out)
    hidden_grad = d_hidden.astype(jnp.float32)
    d_conv = hidden_grad * up_b.astype(jnp.float32) * gelu_slope
    d_up_b = (hidden_grad * gelu_value).astype(jnp.bfloat16)
    later = shifted(d_conv[:span], "fs", -1)
    d_extended = jnp.concatenate([d_conv, later], 0)
    d_up_a = sum(
        (taps_own[i][None, :] * d_extended[span - i : span - i + rows] for i in range(TAPS))
    ).astype(jnp.bfloat16)
    tap_terms = [jnp.sum(d_conv * extended[i : i + rows], axis=0) for i in range(TAPS)]
    column_part = jnp.stack(tap_terms + [jnp.sum(d_conv, axis=0)], 0)
    contract = (((1,), (1,)), ((), ()))
    partial_sum = lax.dot_general(d_up_a, conv_weight, contract, preferred_element_type=jnp.float32)
    partial_sum = partial_sum + lax.dot_general(
        d_up_b, gate_weight, contract, preferred_element_type=jnp.float32
    )
    grad_inputs = lax.psum_scatter(
        partial_sum.astype(jnp.bfloat16), "tp", scatter_dimension=1, tiled=True
    )
    columns = features
    grad_conv_up = lax.psum_scatter(
        lax.dot_general(
            columns, d_up_a, (((0,), (0,)), ((), ())), preferred_element_type=jnp.float32
        ),
        "fs",
        scatter_dimension=0,
        tiled=True,
    )
    squares = jnp.sum(grad_conv_up * grad_conv_up, axis=0)
    placed = jnp.zeros((TAPS + 1, width * lax.axis_size("tp")), jnp.float32)
    placed = lax.dynamic_update_slice_in_dim(placed, column_part, col_start, 1)
    full_columns = lax.psum(placed, ("fs", "tp"))
    unit_norms = lax.psum(squares, "fs")
    return (grad_inputs, grad_conv_up, unit_norms, full_columns[:TAPS], full_columns[TAPS])


def ring_member(place, n):
    depth = n // 2
    place = lax.rem(place + 2 * n, n)
    side = place // depth
    along = lax.rem(place, depth)
    return (side * (depth - 1) + (1 - 2 * side) * along) * 2 + side


def ring_place(index, n):
    side = lax.rem(index, 2)
    along = index // 2
    return side * (n - 1 - 2 * along) + along


def greet(peers):
    barrier = pltpu.get_barrier_semaphore()
    for peer in peers:
        pl.semaphore_signal(barrier, inc=1, device_id=peer, device_id_type=MESH)
    pl.semaphore_wait(barrier, len(peers))


def gather_kernel(n, t, *refs):
    tokens, w_out, t_out = refs[3:5], refs[5:11], refs[11:13]
    send_sem, recv_sem, t_send, t_recv, own_sem = refs[13:]
    cut = w_out[0].shape[2]
    spans = (pl.ds(0, cut), pl.ds(cut, w_out[1].shape[2]))
    weights = [w.at[:, span] for w in refs[:3] for span in spans]
    me, mine = lax.axis_index("fs"), lax.axis_index("tp")
    place = ring_place(me, n)
    ways = (
        {"fs": ring_member(place + 1, n)},
        {"fs": ring_member(place - 1, n)},
    )
    peers = [{"tp": lax.rem(mine + k, t)} for k in range(1, t)]
    greet(list(ways) + peers)
    ring = []
    for step in range(n - 1):
        copies = []
        for i in range(6):
            way = i % 2
            if step:
                ring[step - 1][i].wait_recv()
            owner = ring_member(place - step if way == 0 else place + step, n)
            copy = pltpu.make_async_remote_copy(
                src_ref=w_out[i].at[owner] if step else weights[i],
                dst_ref=w_out[i].at[owner],
                send_sem=send_sem.at[step, i],
                recv_sem=recv_sem.at[step, i],
                device_id=ways[way],
                device_id_type=MESH,
            )
            copy.start()
            copies.append(copy)
        ring.append(copies)
        if step == 0:
            across = []
            for i in range(2):
                for k in range(1, t):
                    copy = pltpu.make_async_remote_copy(
                        src_ref=tokens[i],
                        dst_ref=t_out[i].at[mine],
                        send_sem=t_send.at[i, k - 1],
                        recv_sem=t_recv.at[i, k - 1],
                        device_id=peers[k - 1],
                        device_id_type=MESH,
                    )
                    copy.start()
                    across.append(copy)
            own = [
                pltpu.make_async_copy(weights[i], w_out[i].at[me], own_sem.at[i])
                for i in range(6)
            ] + [
                pltpu.make_async_copy(tokens[i], t_out[i].at[mine], own_sem.at[6 + i])
                for i in range(2)
            ]
            for copy in own:
                copy.start()
    for copy in ring[-1]:
        copy.wait_recv()
    for copy in across:
        copy.wait_recv()
    for copies in ring:
        for copy in copies:
            copy.wait_send()
    for copy in across:
        copy.wait_send()
    for copy in own:
        copy.wait()


def gather_all(weights, tokens, cuts, n, t):
    shape = jax.ShapeDtypeStruct
    return pl.pallas_call(
        functools.partial(gather_kernel, n, t),
        out_shape=[shape((n, w.shape[0], c), w.dtype) for w in weights for c in cuts]
        + [shape((t,) + x.shape, x.dtype) for x in tokens],
        in_specs=[VMEM] * 5,
        out_specs=[ANY] * 8,
        scratch_shapes=[
            pltpu.SemaphoreType.DMA((n - 1, 6)),
            pltpu.SemaphoreType.DMA((n - 1, 6)),
            pltpu.SemaphoreType.DMA((2, t - 1)),
            pltpu.SemaphoreType.DMA((2, t - 1)),
            pltpu.SemaphoreType.DMA((8,)),
        ],
        compiler_params=pltpu.CompilerParams(collective_id=0, has_side_effects=True),
        name="gather_all",
    )(*weights, *tokens)


def reduce_kernel(n, t, *refs):
    grads, partial, columns = refs[:2], refs[2], refs[3]
    g_out, i_out, norm_out, col_out = refs[4:8]
    sent, held = refs[8:10], refs[10:12]
    arrived, col_all, col_sum, norm_own, norm_all = refs[12:17]
    (send_sem, recv_sem, t_send, t_recv, c_send, c_recv, s_send, s_recv, n_send, n_recv) = refs[17:]
    parts = grads[0].shape[1]
    me, mine = lax.axis_index("fs"), lax.axis_index("tp")
    place = ring_place(me, n)
    ways = (
        {"fs": ring_member(place + 1, n)},
        {"fs": ring_member(place - 1, n)},
    )
    peers = [{"tp": lax.rem(mine + k, t)} for k in range(1, t)]
    column = [{"fs": lax.rem(me + k, n)} for k in range(1, n)]
    greet(column + peers)

    def push(src, dst, send, recv, to):
        copy = pltpu.make_async_remote_copy(
            src_ref=src, dst_ref=dst, send_sem=send, recv_sem=recv,
            device_id=to, device_id_type=MESH,
        )
        copy.start()
        return copy

    col_pushes = [
        push(columns, col_all.at[me], c_send.at[k], c_recv.at[k], column[k])
        for k in range(n - 1)
    ]
    across = [
        push(
            partial.at[lax.rem(mine + k, t)],
            arrived.at[k - 1],
            t_send.at[k - 1],
            t_recv.at[k - 1],
            peers[k - 1],
        )
        for k in range(1, t)
    ]
    ring = []
    for step in range(n - 1):
        copies = []
        for c in range(parts):
            for way in range(2):
                ahead = place - 1 - step if way == 0 else place + 1 + step
                value = grads[way][ring_member(ahead, n), c]
                slot = c * 2 + way
                if step:
                    ring[step - 1][slot].wait_recv()
                    value = value + held[way][step - 1, c].astype(jnp.float32)
                sent[way][step, c] = value.astype(jnp.bfloat16)
                copies.append(
                    push(
                        sent[way].at[step, c],
                        held[way].at[step, c],
                        send_sem.at[step, slot],
                        recv_sem.at[step, slot],
                        ways[way],
                    )
                )
        ring.append(copies)
        if step == 1:
            for copy in col_pushes:
                copy.wait_recv()
            total = jnp.zeros(columns.shape, jnp.float32)
            for k in range(n):
                total = total + jnp.where(me == k, columns[...], col_all[k])
            col_sum[...] = total
            col_out[mine] = total
            sum_pushes = [
                push(col_sum, col_out.at[mine], s_send.at[k], s_recv.at[k], peers[k])
                for k in range(t - 1)
            ]
    for copy in across:
        copy.wait_recv()
    rows = partial.shape[1]
    piece = 16 if rows % 16 == 0 else 8

    @pl.loop(0, rows // piece)
    def _(r):
        at = pl.ds(pl.multiple_of(r * piece, piece), piece)
        total = partial[mine, at, :].astype(jnp.float32)
        for k in range(t - 1):
            total = total + arrived[k, at, :].astype(jnp.float32)
        i_out[at, :] = total.astype(jnp.bfloat16)

    height = grads[0].shape[2]
    start = 0
    for way in range(2):
        lanes = grads[way].shape[3]
        squares = jnp.zeros((1, lanes), jnp.float32)
        for c in range(parts):
            slot = c * 2 + way
            ring[-1][slot].wait_recv()
            value = grads[way][me, c] + held[way][n - 2, c].astype(jnp.float32)
            g_out[c * height : (c + 1) * height, start : start + lanes] = value
            squares = squares + jnp.sum(value * value, axis=0, keepdims=True)
        norm_own[:, start : start + lanes] = squares
        start += lanes
    norm_pushes = [
        push(norm_own, norm_all.at[me], n_send.at[k], n_recv.at[k], column[k])
        for k in range(n - 1)
    ]
    for copy in norm_pushes:
        copy.wait_recv()
    total = jnp.zeros(norm_own.shape, jnp.float32)
    for k in range(n):
        total = total + jnp.where(me == k, norm_own[...], norm_all[k])
    norm_out[...] = total
    for copy in sum_pushes:
        copy.wait_recv()
    for copies in ring + [across, col_pushes, sum_pushes, norm_pushes]:
        for copy in copies:
            copy.wait_send()


def reduce_all(grads, partial, columns, n, t):
    shape = jax.ShapeDtypeStruct
    parts, rows = grads[0].shape[1:3]
    width = sum(g.shape[3] for g in grads)
    dma = pltpu.SemaphoreType.DMA
    blocks = [pltpu.VMEM((n - 1,) + g.shape[1:], jnp.bfloat16) for g in grads]
    return pl.pallas_call(
        functools.partial(reduce_kernel, n, t),
        out_shape=[
            shape((parts * rows, width), jnp.float32),
            shape(partial.shape[1:], jnp.bfloat16),
            shape((1, width), jnp.float32),
            shape((t,) + columns.shape, jnp.float32),
        ],
        in_specs=[VMEM] * 4,
        out_specs=[VMEM] * 4,
        scratch_shapes=[
            *blocks,
            *blocks,
            pltpu.VMEM((t - 1,) + partial.shape[1:], jnp.bfloat16),
            pltpu.VMEM((n,) + columns.shape, jnp.float32),
            pltpu.VMEM(columns.shape, jnp.float32),
            pltpu.VMEM((1, width), jnp.float32),
            pltpu.VMEM((n, 1, width), jnp.float32),
            dma((n - 1, 2 * parts)),
            dma((n - 1, 2 * parts)),
            dma((t - 1,)),
            dma((t - 1,)),
            dma((n - 1,)),
            dma((n - 1,)),
            dma((t - 1,)),
            dma((t - 1,)),
            dma((n - 1,)),
            dma((n - 1,)),
        ],
        compiler_params=pltpu.CompilerParams(
            collective_id=1, has_side_effects=True, vmem_limit_bytes=56 * 1024 * 1024
        ),
        name="reduce_all",
    )(*grads, partial, columns)


def halo_kernel(n, block, out, send_sem, recv_sem):
    me = lax.axis_index("fs")
    before, after = {"fs": lax.rem(me + n - 1, n)}, {"fs": lax.rem(me + 1, n)}
    greet([before, after])
    copy = pltpu.make_async_remote_copy(
        src_ref=block, dst_ref=out, send_sem=send_sem, recv_sem=recv_sem,
        device_id=before, device_id_type=MESH,
    )
    copy.start()
    copy.wait()


def from_next(block, n):
    got = pl.pallas_call(
        functools.partial(halo_kernel, n),
        out_shape=jax.ShapeDtypeStruct(block.shape, block.dtype),
        in_specs=[VMEM],
        out_specs=VMEM,
        scratch_shapes=[pltpu.SemaphoreType.DMA, pltpu.SemaphoreType.DMA],
        compiler_params=pltpu.CompilerParams(
            collective_id=2, has_side_effects=True, vmem_limit_bytes=1024 * 1024
        ),
        name="from_next",
    )(block)
    return jnp.where(lax.axis_index("fs") == n - 1, 0.0, got)


def with_kernels(inputs, w_conv_up, w_gate_up, w_down, taps, conv_bias, cotangent):
    n, t = lax.axis_size("fs"), lax.axis_size("tp")
    span = TAPS - 1
    rows = inputs.shape[0]
    shard, width = w_conv_up.shape
    half = -(-width // (2 * LANES)) * LANES
    col_start = lax.axis_index("tp") * width
    cuts = (half, width - half)
    starts = ((0, half), (half, width))
    taps_own = lax.dynamic_slice_in_dim(taps, col_start, width, 1)
    bias_own = lax.dynamic_slice_in_dim(conv_bias, col_start, width, 0)
    got = gather_all([w_down.T, w_conv_up, w_gate_up], [inputs.T, cotangent.T], cuts, n, t)
    down, conv, gate = [[g.reshape(n * shard, -1) for g in got[i : i + 2]] for i in (0, 2, 4)]
    features, cot_full = [g.reshape(-1, rows) for g in got[6:]]

    def project(left, right):
        dots = [
            lax.dot_general(
                left, r, (((0,), (0,)), ((), ())), preferred_element_type=jnp.float32
            ).astype(jnp.bfloat16)
            for r in right
        ]
        return jnp.concatenate(dots, 1)

    up_a = project(features, conv)
    earlier = shifted(up_a[rows - span :], "fs", 1)
    d_hidden = project(cot_full, down)
    up_b = project(features, gate)
    extended = jnp.concatenate([earlier, up_a], 0).astype(jnp.float32)
    conv_out = bias_own[None, :] + sum(
        (taps_own[i][None, :] * extended[i : i + rows] for i in range(TAPS))
    )
    gelu_value, gelu_slope = gelu_parts(conv_out)
    hidden_grad = d_hidden.astype(jnp.float32)
    d_conv = hidden_grad * up_b.astype(jnp.float32) * gelu_slope
    d_up_b = (hidden_grad * gelu_value).astype(jnp.bfloat16)
    later = from_next(d_conv[:8], n)[:span]
    d_extended = jnp.concatenate([d_conv, later], 0)
    d_up_a = sum(
        (taps_own[i][None, :] * d_extended[span - i : span - i + rows] for i in range(TAPS))
    ).astype(jnp.bfloat16)
    tap_terms = [jnp.sum(d_conv * extended[i : i + rows], axis=0) for i in range(TAPS)]
    column_part = jnp.stack(tap_terms + [jnp.sum(d_conv, axis=0)], 0)
    partial_sum = 0.0
    for weight, grad in ((conv, d_up_a), (gate, d_up_b)):
        for h in range(2):
            partial_sum = partial_sum + lax.dot_general(
                weight[h],
                grad[:, slice(*starts[h])],
                (((1,), (1,)), ((), ())),
                preferred_element_type=jnp.float32,
            )
    partial = partial_sum.astype(jnp.bfloat16).reshape(t, -1, rows)
    parts = next(p for p in (3, 4, 2, 1) if shard % (8 * p) == 0)
    grads = [
        jnp.dot(
            features, d_up_a[:, slice(*starts[h])], preferred_element_type=jnp.float32
        ).reshape(n, parts, shard // parts, cuts[h])
        for h in range(2)
    ]
    grad_conv_up, grad_inputs, norms, columns = reduce_all(grads, partial, column_part, n, t)
    full = columns.transpose(1, 0, 2).reshape(TAPS + 1, t * width)
    return (grad_inputs.T, grad_conv_up, norms[0], full[:TAPS], full[TAPS])


def per_device(inputs, w_conv_up, *rest):
    n, t = lax.axis_size("fs"), lax.axis_size("tp")
    aligned = w_conv_up.shape[0] % 8 == 0 and inputs.shape[1] % 8 == 0
    small = n % 2 == 0 and 4 <= n <= 16 and 2 <= t <= 8
    chosen = with_kernels if aligned and small else with_collectives
    return chosen(inputs, w_conv_up, *rest)


def solution(mesh):
    return jax.shard_map(
        per_device,
        mesh=mesh,
        in_specs=(
            P("fs", "tp"),
            P("fs", "tp"),
            P("fs", "tp"),
            P("tp", "fs"),
            P(),
            P(),
            P("fs", "tp"),
        ),
        out_specs=(P("fs", "tp"), P("fs", "tp"), P("tp"), P(), P()),
        check_vma=False,
    )
```

```python
import functools
import math

import jax
import jax.numpy as jnp
from jax import lax
from jax.experimental import pallas as pl
from jax.experimental.pallas import tpu as pltpu
from jax.sharding import PartitionSpec as P

TAPS = 3
LANES = 128
MESH = pl.DeviceIdType.MESH
VMEM = pl.BlockSpec(memory_space=pltpu.VMEM)
ANY = pl.BlockSpec(memory_space=pl.ANY)


def shifted(block, axis, distance):
    devices = range(lax.axis_size(axis))
    route = [(i - distance, i) for i in devices if i - distance in devices]
    return lax.ppermute(block, axis, route)


def gelu_parts(value):
    normal_cdf = 0.5 * (1.0 + jax.scipy.special.erf(value / math.sqrt(2.0)))
    density = jnp.exp(-0.5 * value * value) / math.sqrt(2.0 * math.pi)
    return (value * normal_cdf, normal_cdf + value * density)


def with_collectives(inputs, w_conv_up, w_gate_up, w_down, taps, conv_bias, cotangent):
    span = TAPS - 1
    rows = inputs.shape[0]
    width = w_conv_up.shape[1]
    col_start = lax.axis_index("tp") * width
    taps_own = lax.dynamic_slice_in_dim(taps, col_start, width, 1)
    bias_own = lax.dynamic_slice_in_dim(conv_bias, col_start, width, 0)
    features, cot_full = (
        lax.all_gather(inputs, "tp", axis=1, tiled=True),
        lax.all_gather(cotangent, "tp", axis=1, tiled=True),
    )
    conv_weight, gate_weight = (
        lax.all_gather(w_conv_up, "fs", axis=0, tiled=True),
        lax.all_gather(w_gate_up, "fs", axis=0, tiled=True),
    )
    columns = cot_full
    d_hidden = lax.dot_general(
        columns,
        lax.all_gather(w_down, "fs", axis=1, tiled=True),
        (((1,), (1,)), ((), ())),
        preferred_element_type=jnp.float32,
    ).astype(jnp.bfloat16)
    up_a = jnp.dot(features, conv_weight, preferred_element_type=jnp.float32).astype(jnp.bfloat16)
    up_b = jnp.dot(features, gate_weight, preferred_element_type=jnp.float32).astype(jnp.bfloat16)
    earlier = shifted(up_a[rows - span :], "fs", 1)
    extended = jnp.concatenate([earlier, up_a], 0).astype(jnp.float32)
    conv_out = bias_own[None, :] + sum(
        (taps_own[i][None, :] * extended[i : i + rows] for i in range(TAPS))
    )
    gelu_value, gelu_slope = gelu_parts(conv_out)
    hidden_grad = d_hidden.astype(jnp.float32)
    d_conv = hidden_grad * up_b.astype(jnp.float32) * gelu_slope
    d_up_b = (hidden_grad * gelu_value).astype(jnp.bfloat16)
    later = shifted(d_conv[:span], "fs", -1)
    d_extended = jnp.concatenate([d_conv, later], 0)
    d_up_a = sum(
        (taps_own[i][None, :] * d_extended[span - i : span - i + rows] for i in range(TAPS))
    ).astype(jnp.bfloat16)
    tap_terms = [jnp.sum(d_conv * extended[i : i + rows], axis=0) for i in range(TAPS)]
    column_part = jnp.stack(tap_terms + [jnp.sum(d_conv, axis=0)], 0)
    contract = (((1,), (1,)), ((), ()))
    partial_sum = lax.dot_general(d_up_a, conv_weight, contract, preferred_element_type=jnp.float32)
    partial_sum = partial_sum + lax.dot_general(
        d_up_b, gate_weight, contract, preferred_element_type=jnp.float32
    )
    grad_inputs = lax.psum_scatter(
        partial_sum.astype(jnp.bfloat16), "tp", scatter_dimension=1, tiled=True
    )
    columns = features
    grad_conv_up = lax.psum_scatter(
        lax.dot_general(
            columns, d_up_a, (((0,), (0,)), ((), ())), preferred_element_type=jnp.float32
        ),
        "fs",
        scatter_dimension=0,
        tiled=True,
    )
    squares = jnp.sum(grad_conv_up * grad_conv_up, axis=0)
    placed = jnp.zeros((TAPS + 1, width * lax.axis_size("tp")), jnp.float32)
    placed = lax.dynamic_update_slice_in_dim(placed, column_part, col_start, 1)
    full_columns = lax.psum(placed, ("fs", "tp"))
    unit_norms = lax.psum(squares, "fs")
    return (grad_inputs, grad_conv_up, unit_norms, full_columns[:TAPS], full_columns[TAPS])


def ring_member(place, n):
    depth = n // 2
    place = lax.rem(place + 2 * n, n)
    side = place // depth
    along = lax.rem(place, depth)
    return (side * (depth - 1) + (1 - 2 * side) * along) * 2 + side


def ring_place(index, n):
    side = lax.rem(index, 2)
    along = index // 2
    return side * (n - 1 - 2 * along) + along


def greet(peers):
    barrier = pltpu.get_barrier_semaphore()
    for peer in peers:
        pl.semaphore_signal(barrier, inc=1, device_id=peer, device_id_type=MESH)
    pl.semaphore_wait(barrier, len(peers))


def gather_kernel(n, t, *refs):
    tokens, grown, projected = refs[3:5], refs[5:10], refs[10:13]
    w_out = refs[13:15] + grown[:4]
    t_out = (grown[4], refs[15])
    totals = refs[16:22]
    send_sem, recv_sem, t_send, t_recv = refs[22:]
    cut, rest = w_out[0].shape[2], w_out[1].shape[2]
    spans = (pl.ds(0, cut), pl.ds(cut, rest))
    weights = [w.at[:, span] for w in refs[:3] for span in spans]
    me, mine = lax.axis_index("fs"), lax.axis_index("tp")
    place = ring_place(me, n)
    ways = (
        {"fs": ring_member(place + 1, n)},
        {"fs": ring_member(place - 1, n)},
    )
    peers = [{"tp": lax.rem(mine + k, t)} for k in range(1, t)]
    blocks = tokens[0].shape[0]
    held = pl.ds(mine * blocks, blocks)
    greet(list(ways) + peers)

    def push(src, dst, send, recv, to):
        copy = pltpu.make_async_remote_copy(
            src_ref=src, dst_ref=dst, send_sem=send, recv_sem=recv,
            device_id=to, device_id_type=MESH,
        )
        copy.start()
        return copy

    def owner_of(i, step):
        return ring_member(place - step if i % 2 == 0 else place + step, n)

    def multiply(step, i):
        owner = owner_of(i, step)
        product = lax.dot_general(
            t_out[1 if i < 2 else 0][owner],
            w_out[i][owner],
            (((0,), (0,)), ((), ())),
            preferred_element_type=jnp.float32,
        )
        totals[i][...] = totals[i][...] + product if step else product

    first = min(3, n - 2)
    waiting = [(step, i) for step in range(n) for i in range(6)]
    ring = []
    for step in range(n - 1):
        copies = []
        for i in range(6):
            if step:
                ring[step - 1][i].wait_recv()
            owner = owner_of(i, step)
            copies.append(
                push(
                    w_out[i].at[owner] if step else weights[i],
                    w_out[i].at[owner],
                    send_sem.at[step, i],
                    recv_sem.at[step, i],
                    ways[i % 2],
                )
            )
            if step == first and i == 0:
                for copy in across:
                    copy.wait_recv()
            if step >= first:
                for _ in range(2):
                    if waiting[0] <= (step, i):
                        multiply(*waiting.pop(0))
        ring.append(copies)
        if step == 0:
            across = [
                push(
                    tokens[i],
                    t_out[i].at[held],
                    t_send.at[i, k - 1],
                    t_recv.at[i, k - 1],
                    peers[k - 1],
                )
                for i in range(2)
                for k in range(1, t)
            ]
            for i in range(6):
                w_out[i][me] = refs[i // 2][:, (i % 2) * cut : cut + (i % 2) * rest]
            for i in range(2):
                t_out[i][held] = tokens[i][...]
    for step, i in waiting:
        if step == n - 1:
            ring[-1][i].wait_recv()
        multiply(step, i)
    for i in range(6):
        projected[i // 2][:, (i % 2) * cut : cut + (i % 2) * rest] = totals[i][...].astype(
            jnp.bfloat16
        )
    for copies in ring + [across]:
        for copy in copies:
            copy.wait_send()


def gather_all(weights, tokens, cuts, n, t):
    shape, kind = jax.ShapeDtypeStruct, jnp.bfloat16
    shard, width = weights[0].shape
    rows = tokens[0].shape[1]
    tokens = [x.reshape(-1, shard, rows) for x in tokens]
    dma = pltpu.SemaphoreType.DMA
    return pl.pallas_call(
        functools.partial(gather_kernel, n, t),
        out_shape=[shape((n, shard, c), kind) for _ in range(2) for c in cuts]
        + [shape((n, shard, rows), kind)]
        + [shape((rows, width), kind)] * 3,
        in_specs=[VMEM] * 5,
        out_specs=[VMEM] * 8,
        scratch_shapes=[pltpu.VMEM((n, shard, c), kind) for c in cuts]
        + [pltpu.VMEM((n, shard, rows), kind)]
        + [pltpu.VMEM((rows, c), jnp.float32) for _ in range(3) for c in cuts]
        + [dma((n - 1, 6)), dma((n - 1, 6)), dma((2, t - 1)), dma((2, t - 1))],
        compiler_params=pltpu.CompilerParams(
            collective_id=0, has_side_effects=True, vmem_limit_bytes=56 * 1024 * 1024
        ),
        name="gather_all",
    )(*weights, *tokens)


def reduce_kernel(n, t, *refs):
    grads, partial, columns = refs[:2], refs[2], refs[3]
    g_out, i_out, norm_out, col_out = refs[4:8]
    sent, held = refs[8:10], refs[10:12]
    arrived, col_all, col_sum, norm_own, norm_all = refs[12:17]
    (send_sem, recv_sem, t_send, t_recv, c_send, c_recv, s_send, s_recv, n_send, n_recv) = refs[17:]
    parts = grads[0].shape[1]
    me, mine = lax.axis_index("fs"), lax.axis_index("tp")
    place = ring_place(me, n)
    ways = (
        {"fs": ring_member(place + 1, n)},
        {"fs": ring_member(place - 1, n)},
    )
    peers = [{"tp": lax.rem(mine + k, t)} for k in range(1, t)]
    column = [{"fs": lax.rem(me + k, n)} for k in range(1, n)]
    greet(column + peers)

    def push(src, dst, send, recv, to):
        copy = pltpu.make_async_remote_copy(
            src_ref=src, dst_ref=dst, send_sem=send, recv_sem=recv,
            device_id=to, device_id_type=MESH,
        )
        copy.start()
        return copy

    col_pushes = [
        push(columns, col_all.at[me], c_send.at[k], c_recv.at[k], column[k])
        for k in range(n - 1)
    ]
    across = [
        push(
            partial.at[lax.rem(mine + k, t)],
            arrived.at[k - 1],
            t_send.at[k - 1],
            t_recv.at[k - 1],
            peers[k - 1],
        )
        for k in range(1, t)
    ]
    ring = []
    for step in range(n - 1):
        copies = []
        for c in range(parts):
            for way in range(2):
                ahead = place - 1 - step if way == 0 else place + 1 + step
                value = grads[way][ring_member(ahead, n), c]
                slot = c * 2 + way
                if step:
                    ring[step - 1][slot].wait_recv()
                    value = value + held[way][step - 1, c].astype(jnp.float32)
                sent[way][step, c] = value.astype(jnp.bfloat16)
                copies.append(
                    push(
                        sent[way].at[step, c],
                        held[way].at[step, c],
                        send_sem.at[step, slot],
                        recv_sem.at[step, slot],
                        ways[way],
                    )
                )
        ring.append(copies)
        if step == 1:
            for copy in col_pushes:
                copy.wait_recv()
            total = jnp.zeros(columns.shape, jnp.float32)
            for k in range(n):
                total = total + jnp.where(me == k, columns[...], col_all[k])
            col_sum[...] = total
            col_out[mine] = total
            sum_pushes = [
                push(col_sum, col_out.at[mine], s_send.at[k], s_recv.at[k], peers[k])
                for k in range(t - 1)
            ]
    for copy in across:
        copy.wait_recv()
    rows = partial.shape[1]
    piece = 16 if rows % 16 == 0 else 8

    @pl.loop(0, rows // piece)
    def _(r):
        at = pl.ds(pl.multiple_of(r * piece, piece), piece)
        total = partial[mine, at, :].astype(jnp.float32)
        for k in range(t - 1):
            total = total + arrived[k, at, :].astype(jnp.float32)
        i_out[at, :] = total.astype(jnp.bfloat16)

    height = grads[0].shape[2]
    start = 0
    for way in range(2):
        lanes = grads[way].shape[3]
        squares = jnp.zeros((1, lanes), jnp.float32)
        for c in range(parts):
            slot = c * 2 + way
            ring[-1][slot].wait_recv()
            value = grads[way][me, c] + held[way][n - 2, c].astype(jnp.float32)
            g_out[c * height : (c + 1) * height, start : start + lanes] = value
            squares = squares + jnp.sum(value * value, axis=0, keepdims=True)
        norm_own[:, start : start + lanes] = squares
        start += lanes
    norm_pushes = [
        push(norm_own, norm_all.at[me], n_send.at[k], n_recv.at[k], column[k])
        for k in range(n - 1)
    ]
    for copy in norm_pushes:
        copy.wait_recv()
    total = jnp.zeros(norm_own.shape, jnp.float32)
    for k in range(n):
        total = total + jnp.where(me == k, norm_own[...], norm_all[k])
    norm_out[...] = total
    for copy in sum_pushes:
        copy.wait_recv()
    for copies in ring + [across, col_pushes, sum_pushes, norm_pushes]:
        for copy in copies:
            copy.wait_send()


def reduce_all(grads, partial, columns, n, t):
    shape = jax.ShapeDtypeStruct
    parts, rows = grads[0].shape[1:3]
    width = sum(g.shape[3] for g in grads)
    dma = pltpu.SemaphoreType.DMA
    blocks = [pltpu.VMEM((n - 1,) + g.shape[1:], jnp.bfloat16) for g in grads]
    return pl.pallas_call(
        functools.partial(reduce_kernel, n, t),
        out_shape=[
            shape((parts * rows, width), jnp.float32),
            shape(partial.shape[1:], jnp.bfloat16),
            shape((1, width), jnp.float32),
            shape((t,) + columns.shape, jnp.float32),
        ],
        in_specs=[VMEM] * 4,
        out_specs=[VMEM] * 4,
        scratch_shapes=[
            *blocks,
            *blocks,
            pltpu.VMEM((t - 1,) + partial.shape[1:], jnp.bfloat16),
            pltpu.VMEM((n,) + columns.shape, jnp.float32),
            pltpu.VMEM(columns.shape, jnp.float32),
            pltpu.VMEM((1, width), jnp.float32),
            pltpu.VMEM((n, 1, width), jnp.float32),
            dma((n - 1, 2 * parts)),
            dma((n - 1, 2 * parts)),
            dma((t - 1,)),
            dma((t - 1,)),
            dma((n - 1,)),
            dma((n - 1,)),
            dma((t - 1,)),
            dma((t - 1,)),
            dma((n - 1,)),
            dma((n - 1,)),
        ],
        compiler_params=pltpu.CompilerParams(
            collective_id=1, has_side_effects=True, vmem_limit_bytes=56 * 1024 * 1024
        ),
        name="reduce_all",
    )(*grads, partial, columns)


def halo_kernel(n, block, out, send_sem, recv_sem):
    me = lax.axis_index("fs")
    before, after = {"fs": lax.rem(me + n - 1, n)}, {"fs": lax.rem(me + 1, n)}
    greet([before, after])
    copy = pltpu.make_async_remote_copy(
        src_ref=block, dst_ref=out, send_sem=send_sem, recv_sem=recv_sem,
        device_id=before, device_id_type=MESH,
    )
    copy.start()
    copy.wait()


def from_next(block, n):
    got = pl.pallas_call(
        functools.partial(halo_kernel, n),
        out_shape=jax.ShapeDtypeStruct(block.shape, block.dtype),
        in_specs=[VMEM],
        out_specs=VMEM,
        scratch_shapes=[pltpu.SemaphoreType.DMA, pltpu.SemaphoreType.DMA],
        compiler_params=pltpu.CompilerParams(
            collective_id=2, has_side_effects=True, vmem_limit_bytes=1024 * 1024
        ),
        name="from_next",
    )(block)
    return jnp.where(lax.axis_index("fs") == n - 1, 0.0, got)


def with_kernels(inputs, w_conv_up, w_gate_up, w_down, taps, conv_bias, cotangent):
    n, t = lax.axis_size("fs"), lax.axis_size("tp")
    span = TAPS - 1
    rows = inputs.shape[0]
    shard, width = w_conv_up.shape
    half = -(-width // (2 * LANES)) * LANES
    col_start = lax.axis_index("tp") * width
    cuts = (half, width - half)
    starts = ((0, half), (half, width))
    taps_own = lax.dynamic_slice_in_dim(taps, col_start, width, 1)
    bias_own = lax.dynamic_slice_in_dim(conv_bias, col_start, width, 0)
    got = gather_all([w_down.T, w_conv_up, w_gate_up], [inputs.T, cotangent.T], cuts, n, t)
    conv, gate = [[g.reshape(n * shard, -1) for g in got[i : i + 2]] for i in (0, 2)]
    features = got[4].reshape(-1, rows)
    d_hidden, up_a, up_b = got[5:]
    earlier = shifted(up_a[rows - span :], "fs", 1)
    extended = jnp.concatenate([earlier, up_a], 0).astype(jnp.float32)
    conv_out = bias_own[None, :] + sum(
        (taps_own[i][None, :] * extended[i : i + rows] for i in range(TAPS))
    )
    gelu_value, gelu_slope = gelu_parts(conv_out)
    hidden_grad = d_hidden.astype(jnp.float32)
    d_conv = hidden_grad * up_b.astype(jnp.float32) * gelu_slope
    d_up_b = (hidden_grad * gelu_value).astype(jnp.bfloat16)
    later = from_next(d_conv[:8], n)[:span]
    d_extended = jnp.concatenate([d_conv, later], 0)
    d_up_a = sum(
        (taps_own[i][None, :] * d_extended[span - i : span - i + rows] for i in range(TAPS))
    ).astype(jnp.bfloat16)
    tap_terms = [jnp.sum(d_conv * extended[i : i + rows], axis=0) for i in range(TAPS)]
    column_part = jnp.stack(tap_terms + [jnp.sum(d_conv, axis=0)], 0)
    partial_sum = 0.0
    for weight, grad in ((conv, d_up_a), (gate, d_up_b)):
        for h in range(2):
            partial_sum = partial_sum + lax.dot_general(
                weight[h],
                grad[:, slice(*starts[h])],
                (((1,), (1,)), ((), ())),
                preferred_element_type=jnp.float32,
            )
    partial = partial_sum.astype(jnp.bfloat16).reshape(t, -1, rows)
    parts = next(p for p in (3, 4, 2, 1) if shard % (8 * p) == 0)
    grads = [
        jnp.dot(
            features, d_up_a[:, slice(*starts[h])], preferred_element_type=jnp.float32
        ).reshape(n, parts, shard // parts, cuts[h])
        for h in range(2)
    ]
    grad_conv_up, grad_inputs, norms, columns = reduce_all(grads, partial, column_part, n, t)
    full = columns.transpose(1, 0, 2).reshape(TAPS + 1, t * width)
    return (grad_inputs.T, grad_conv_up, norms[0], full[:TAPS], full[TAPS])


def per_device(inputs, w_conv_up, *rest):
    n, t = lax.axis_size("fs"), lax.axis_size("tp")
    aligned = w_conv_up.shape[0] % 8 == 0 and inputs.shape[1] % w_conv_up.shape[0] == 0
    small = n % 2 == 0 and 4 <= n <= 16 and 2 <= t <= 8
    chosen = with_kernels if aligned and small else with_collectives
    return chosen(inputs, w_conv_up, *rest)


def solution(mesh):
    return jax.shard_map(
        per_device,
        mesh=mesh,
        in_specs=(
            P("fs", "tp"),
            P("fs", "tp"),
            P("fs", "tp"),
            P("tp", "fs"),
            P(),
            P(),
            P("fs", "tp"),
        ),
        out_specs=(P("fs", "tp"), P("fs", "tp"), P("tp"), P(), P()),
        check_vma=False,
    )
```
